32 devices in a mesh: ep: 8 (over z, x), tp: 4 (over y, core).
Axes of the slice: x: 2, y: 2, z: 4, core: 2. Of those that a mesh axis runs over, the one named last changes fastest.
Arguments:
- queries: bfloat16 [4096, 2048], P('ep', 'tp'), may hold values from -5 to 5
- key_rows: bfloat16 [4096, 2048], P('ep', 'tp'), may hold values from -5 to 5
- values: bfloat16 [4096, 2048], P('ep', 'tp'), may hold values from -6 to 6
- forget_log: float32 [4096, 16], P(None, 'tp'), may hold values from -515 to 0, as said below
- out_weight: bfloat16 [2048, 4096], P(None, 'tp'), may hold values from -1 to 1
- expert_input: bfloat16 [1024, 4096], P(('ep', 'tp')), may hold values from -6 to 6
- norm_gain: float32 [4096], replicated, may hold values from 0.1 to 1.9
- route_ids: int32 [1024, 2], P('ep'), may hold values from 0 to 7, all different within a row; in each aligned block of 128 rows (0 to 127, 128 to 255, ...) at most 64 rows name the same one
- route_weights: float32 [1024, 2], P('ep'), may hold values from 0.2 to 1
- gate_weight: bfloat16 [8, 4096, 2048], P('ep', None, 'tp'), may hold values from -0.09375 to 0.09375
- up_weight: bfloat16 [8, 4096, 2048], P('ep', None, 'tp'), may hold values from -0.09375 to 0.09375
- down_weight: bfloat16 [8, 2048, 4096], P('ep', None, 'tp'), may hold values from -0.125 to 0.125
Outputs:
- mixer_out: bfloat16 [4096, 4096], P('ep', 'tp')
- expert_out: bfloat16 [1024, 4096], P('ep', 'tp')
The draws below stay inside these ranges and needn't reach their ends.
Inputs may be any that keep to these rules, and one draw needn't show every extreme that they name: forget_log[t, h] is the sum of the log forget gates of head h at positions 0 to t of the one sequence; it never rises along positions. `route_ids`: each row names 2 different experts. In each aligned block of 128 rows (the rows of one index of ep) no expert is named by more than 64 rows, and some block reaches 64.
All inputs are finite; a program needn't handle non-finite values.
Results may differ from the reference program's by a relative error of at most 0.0071.
Values may be sent and summed in bfloat16 or wider, within the bound.
No kernel may reach another device: no remote copies, remote signals or barrier semaphores. Data moves between devices by JAX's collectives and lax.ppermute only.
A program may use at most 64 MiB of HBM per device.

```python
import math
import jax
import jax.numpy as jnp
import numpy as np
from jax import lax

D = 4096
HEAD_COUNT = 16
HD = 128
FFE = 2048
TOPK = 2
ROWS_A = 512
ROWS_B = 128
SEQUENCE_LENGTH = 4096
TOKENS_B = 1024
EXPERTS = 8
CAP = 64
N_EP = 8


def draw_queries(key, part):
    drawn_rows = jnp.clip(1.5 * jax.random.normal(jax.random.fold_in(key, 1), (SEQUENCE_LENGTH, HEAD_COUNT * HD), jnp.float32), -5.0, 5.0)
    return drawn_rows.astype(jnp.bfloat16)


def draw_key_rows(key, part):
    drawn_rows = jnp.clip(jax.random.normal(jax.random.fold_in(key, 2), (SEQUENCE_LENGTH, HEAD_COUNT * HD), jnp.float32), -5.0, 5.0)
    return drawn_rows.astype(jnp.bfloat16)


def draw_forget_log(key, part):
    fast_share = 0.5
    fast_heads = jax.random.uniform(jax.random.fold_in(key, 3), (HEAD_COUNT,), jnp.float32) < fast_share
    slow_rate = jnp.exp(jax.random.uniform(jax.random.fold_in(key, 4), (HEAD_COUNT,), jnp.float32, jnp.log(0.2), jnp.log(0.8))) / SEQUENCE_LENGTH
    fast_rate = jnp.exp(jax.random.uniform(jax.random.fold_in(key, 5), (HEAD_COUNT,), jnp.float32, jnp.log(0.01), jnp.log(1.0 / 30.0)))
    head_rate = jnp.where(fast_heads, fast_rate, slow_rate)
    block_factor = jnp.exp(jax.random.uniform(jax.random.fold_in(key, 6), (SEQUENCE_LENGTH // ROWS_A, HEAD_COUNT), jnp.float32, -0.7, 0.7))
    block_factor = jnp.repeat(block_factor, ROWS_A, axis=0)
    roughness = jax.random.uniform(jax.random.fold_in(key, 7), (SEQUENCE_LENGTH, HEAD_COUNT), jnp.float32, 0.3, 1.7)
    step_logarithm = -head_rate[None, :] * block_factor * roughness
    surge_locations = jax.random.randint(jax.random.fold_in(key, 8), (2, HEAD_COUNT), 0, SEQUENCE_LENGTH)
    position_indices = jnp.arange(SEQUENCE_LENGTH, dtype=jnp.int32)
    surge_matched = jnp.any(position_indices[:, None, None] == surge_locations[None, :, :], axis=1)
    surge_penalty = jnp.log(jax.random.uniform(jax.random.fold_in(key, 9), (SEQUENCE_LENGTH, HEAD_COUNT), jnp.float32, 0.6, 0.8))
    step_logarithm = step_logarithm + jnp.where(surge_matched, surge_penalty, 0.0)
    return jnp.cumsum(step_logarithm, axis=0).astype(jnp.float32)


def block_scale(rng, extent, split, least, top_value):
    factor_of, own = 1.0, jax.random.fold_in(rng, 6)
    for dim, shards_of in split:
        draws = jnp.exp(jax.random.uniform(jax.random.fold_in(own, dim), (shards_of,), jnp.float32, least / len(split), top_value / len(split)))
        factor_of = factor_of * jnp.repeat(draws, extent[dim] // shards_of).reshape([-1 if axis == dim else 1 for axis in range(len(extent))])
    return factor_of


def shared_out(rng, own, number, rows, number_of, top, reach, skew):
    order = jax.random.permutation(rng, number_of)
    heavy_load, usual = load_shares(number_of, rows * top, reach, skew, True), load_shares(number_of, rows * top, reach, skew, False)
    places = jnp.arange(number_of)

    def named(sizes, offset_by):
        used = int((sizes > 0).sum())
        fixed = max(1, used // 4)
        passed = fixed + (places - fixed + offset_by * (used - fixed)) % max(1, number_of - fixed)
        return jnp.zeros((number_of,), jnp.int32).at[order[jnp.where(places < fixed, places, passed)]].set(jnp.asarray(sizes, jnp.int32))

    sizes = jnp.where(number % 4 == 0, named(heavy_load, number // 4), named(usual, number - number // 4 - 1))
    mixed = jax.random.permutation(jax.random.fold_in(own, 3), number_of)
    giver, receiver = mixed[0:number_of // 2 * 2:2], mixed[1:number_of // 2 * 2:2]
    slack = jnp.minimum(sizes[giver] - 1, reach - sizes[receiver]) // 2
    slack = jnp.where((giver == order[0]) | (receiver == order[0]) | (sizes[receiver] == 0), 0, jnp.maximum(slack, 0))
    passed = jax.random.randint(jax.random.fold_in(own, 4), (number_of // 2,), 0, 1 << 20) % (slack + 1)
    sizes = sizes.at[giver].add(-passed).at[receiver].add(passed)
    items = jnp.searchsorted(jnp.cumsum(sizes), jnp.arange(rows * top), side="right").astype(jnp.int32)
    table = items.reshape(top, rows).T
    table = table[jax.random.permutation(jax.random.fold_in(own, 1), rows)]
    offset_by = jax.random.randint(jax.random.fold_in(own, 2), (rows, 1), 0, top)
    return jnp.take_along_axis(table, (jnp.arange(top)[None, :] + offset_by) % top, axis=1)


def load_shares(count, total, limit, slope, full):
    portions = [(1 << 20) // math.isqrt(grade ** slope) + 1 for grade in range(1, count + 1)]
    largest = limit if full else min(limit, max(-(-total // count), total * portions[0] // sum(portions)))
    least = 1 if total - largest >= count - 1 else 0
    counts, rest = [largest] + [least] * (count - 1), total - largest - least * (count - 1)
    while rest > 0:
        movable = [i for i in range(1, count) if counts[i] < largest] or [i for i in range(1, count) if counts[i] < limit]
        mass, left = sum([portions[i] for i in movable]), rest
        for i in movable:
            addition = min(limit - counts[i], max(1, left * portions[i] // mass), rest)
            counts[i] = counts[i] + addition
            rest = rest - addition
    return np.array(counts)


def noise(key, dims, width, most, cuts=(), held_as=jnp.bfloat16):
    factor_of = block_scale(key, dims, cuts, -0.22, 0.18) if cuts else 1.0
    drawn = jax.random.normal(key, dims, jnp.float32) * width * factor_of
    return jnp.minimum(jnp.maximum(drawn, -most), most).astype(held_as)


def setup_inputs(seed: int = 0) -> dict:
    key_list = jax.random.split(jax.random.key(seed), 13)
    queries = draw_queries(jax.random.fold_in(key_list[12], 71), 0)
    key_rows = draw_key_rows(jax.random.fold_in(key_list[12], 71), 0)
    values = noise(key_list[2], (SEQUENCE_LENGTH, HEAD_COUNT * HD), 1.0, 6.0, ((0, 8), (1, 4)))
    forget_log = draw_forget_log(jax.random.fold_in(key_list[12], 71), 0)
    out_weight = noise(key_list[4], (HEAD_COUNT * HD, D), (HD // 4) ** -0.5, 1.0, ((1, 4),))
    expert_input = noise(key_list[5], (TOKENS_B, D), 1.0, 6.0, ((0, 32),))
    norm_gain = jnp.clip(1.0 + 0.18 * jax.random.normal(key_list[6], (D,), jnp.float32), 0.1, 1.9)
    route_ids_keys = jax.random.split(jax.random.fold_in(key_list[7], 1), TOKENS_B // ROWS_B)
    route_ids_turns = jax.random.permutation(jax.random.fold_in(key_list[7], 3), TOKENS_B // ROWS_B)
    route_ids = jax.vmap(lambda own, number: shared_out(jax.random.fold_in(key_list[7], 2), own, number, ROWS_B, EXPERTS, TOPK, CAP, 2))(route_ids_keys, route_ids_turns).reshape((TOKENS_B, TOPK))
    route_weights = jnp.clip(0.2 + 0.8 * jax.random.uniform(key_list[8], (TOKENS_B, TOPK), jnp.float32) ** block_scale(key_list[8], (TOKENS_B, TOPK), ((0, 8),), -0.2, 0.2), 0.2, 1.0)
    gate_weight = noise(key_list[9], (EXPERTS, D, FFE), D ** -0.5, 0.09375, ((0, 8), (2, 4)))
    up_weight = noise(key_list[10], (EXPERTS, D, FFE), D ** -0.5, 0.09375, ((0, 8), (2, 4)))
    down_weight = noise(key_list[11], (EXPERTS, FFE, D), FFE ** -0.5, 0.125, ((0, 8), (2, 4)))
    return {"queries": queries, "key_rows": key_rows, "values": values, "forget_log": forget_log, "out_weight": out_weight, "expert_input": expert_input, "norm_gain": norm_gain, "route_ids": route_ids, "route_weights": route_weights, "gate_weight": gate_weight, "up_weight": up_weight, "down_weight": down_weight}


EPSILON = 1e-05

def slot_places(route_rows, experts, capacity):
    entries = route_rows.reshape(-1).astype(jnp.int32)
    matches = (entries[:, None] == jnp.arange(experts, dtype=jnp.int32)[None, :]).astype(jnp.int32)
    earlier = (jnp.cumsum(matches, axis=0) - matches).astype(jnp.int32)
    ranking = lax.optimization_barrier(jnp.sum(earlier * matches, axis=1)).astype(jnp.int32)
    return (entries * capacity + ranking).astype(jnp.int32)

def reference(queries, key_rows, values, forget_log, out_weight, expert_input, norm_gain, route_ids, route_weights, gate_weight, up_weight, down_weight):
    length_all = queries.shape[0]
    query_heads = queries.reshape(length_all, HEAD_COUNT, HD).astype(jnp.float32)
    key_heads = key_rows.reshape(length_all, HEAD_COUNT, HD).astype(jnp.float32)
    value_heads = values.reshape(length_all, HEAD_COUNT, HD).astype(jnp.float32)
    key_places = jnp.arange(length_all, dtype=jnp.int32)
    score_scale = HD ** (-0.5)

    def attend(block_index):
        block_start = (block_index * ROWS_A).astype(jnp.int32)
        query_block = lax.dynamic_slice_in_dim(query_heads, block_start, ROWS_A, 0)
        gate_block = lax.dynamic_slice_in_dim(forget_log, block_start, ROWS_A, 0)
        scores = jnp.einsum('qhd,khd->hqk', query_block, key_heads) * score_scale
        scores = scores + gate_block.T[:, :, None] - forget_log.T[:, None, :]
        query_places = block_start + jnp.arange(ROWS_A, dtype=jnp.int32)
        scores = jnp.where(key_places[None, None, :] <= query_places[None, :, None], scores, -jnp.inf)
        row_max = lax.optimization_barrier(jnp.max(scores, axis=2, keepdims=True))
        weights_now = jnp.exp(scores - row_max)
        denominator = lax.optimization_barrier(jnp.sum(weights_now, axis=2))
        rounded = lax.optimization_barrier(weights_now.astype(jnp.bfloat16)).astype(jnp.float32)
        numerator = jnp.einsum('hqk,khd->qhd', rounded, value_heads)
        return (numerator / denominator.T[:, :, None]).astype(jnp.bfloat16)
    attended = lax.map(attend, jnp.arange(length_all // ROWS_A, dtype=jnp.int32)).reshape(length_all, HEAD_COUNT * HD)
    mixer_out = jnp.dot(attended, out_weight, preferred_element_type=jnp.float32).astype(jnp.bfloat16)
    as_float = expert_input.astype(jnp.float32)
    center = lax.optimization_barrier(jnp.mean(as_float, axis=1, keepdims=True))
    variance = lax.optimization_barrier(jnp.mean(jnp.square(as_float - center), axis=1, keepdims=True))
    normed = ((as_float - center) * lax.rsqrt(variance + EPSILON) * norm_gain).astype(jnp.bfloat16)
    blocks = route_ids.reshape(N_EP, ROWS_B, TOPK)
    places = jax.vmap(lambda block_ids: slot_places(block_ids, EXPERTS, CAP))(blocks)
    expert_of = blocks.reshape(N_EP, ROWS_B * TOPK).astype(jnp.int32)
    ranking = places - expert_of * CAP
    block_index = jnp.arange(N_EP, dtype=jnp.int32)[:, None]
    global_slot = (expert_of * (N_EP * CAP) + block_index * CAP + ranking).astype(jnp.int32)
    owners = (block_index * ROWS_B + jnp.arange(ROWS_B * TOPK, dtype=jnp.int32)[None, :] // TOPK).astype(jnp.int32)
    slot_table = jnp.full((EXPERTS * N_EP * CAP,), TOKENS_B, jnp.int32).at[global_slot.reshape(-1)].set(owners.reshape(-1))
    slot_table = slot_table.reshape(EXPERTS, N_EP * CAP)

    def run_expert(expert_index):
        chosen_rows = jnp.take(normed, slot_table[expert_index], axis=0, mode='fill', fill_value=0)
        gate_part = jnp.dot(chosen_rows, gate_weight[expert_index], preferred_element_type=jnp.float32)
        up_part = jnp.dot(chosen_rows, up_weight[expert_index], preferred_element_type=jnp.float32)
        hidden = (jax.nn.silu(gate_part) * up_part).astype(jnp.bfloat16)
        return jnp.dot(hidden, down_weight[expert_index], preferred_element_type=jnp.float32).astype(jnp.bfloat16)
    results = lax.map(run_expert, jnp.arange(EXPERTS, dtype=jnp.int32)).reshape(EXPERTS * N_EP * CAP, D)
    picked = jnp.take(results, global_slot.reshape(-1), axis=0).astype(jnp.float32)
    combined = lax.optimization_barrier(jnp.sum((picked * route_weights.reshape(-1)[:, None]).reshape(TOKENS_B, TOPK, D), axis=1))
    return (mixer_out, combined.astype(jnp.bfloat16))
```

```python
import functools
import math

import jax
import jax.numpy as jnp
from jax import lax
from jax.experimental import pallas as pl
from jax.experimental.pallas import tpu as pltpu
from jax.sharding import PartitionSpec as P

EPSILON = 1e-05
LOG2E = math.log2(math.e)
VMEM = pltpu.MemorySpace.VMEM
SMEM = pltpu.MemorySpace.SMEM
HBM = pltpu.MemorySpace.HBM
f32 = jnp.float32
bf16 = jnp.bfloat16


def swap(array, axis, offset):
    size = lax.axis_size(axis)
    return lax.ppermute(array, axis, [(i, i ^ offset) for i in range(size)])


def doubled(array, axis, size, unit=1):
    items = [(0, array)]
    bit = size // 2
    while bit:
        items = items + [(k ^ bit, swap(v, axis, bit * unit)) for k, v in items]
        bit //= 2
    return [k for k, _ in items], [v for _, v in items]


def call(kernel, outs, ins, args, **kw):
    return pl.pallas_call(
        kernel,
        out_shape=outs,
        in_specs=ins,
        compiler_params=pltpu.CompilerParams(vmem_limit_bytes=56 << 20),
        **kw,
    )(*args)


def vm(n):
    return [pl.BlockSpec(memory_space=VMEM)] * n


def slice_kernel(width, groups, ids, q_ref, k_ref, v_ref, *outs):
    own = ids[0]
    for k in range(groups):
        at = pl.ds(pl.multiple_of((own ^ k) * width, width), width)
        outs[k][...] = q_ref[:, at]
        outs[groups + k][:, :width] = k_ref[:, at]
        outs[groups + k][:, width:] = v_ref[:, at]


def flash_kernel(groups, members, offsets, rows, width, ids, *refs):
    count = groups * members
    q_refs = refs[:groups]
    kv_refs = refs[groups : groups + count]
    row_ref, col_ref = refs[groups + count : groups + count + 2]
    o_refs = refs[groups + count + 2 : 2 * groups + count + 2]
    kv, qs, sems = refs[2 * groups + count + 2 :]
    group, member = ids[0], ids[1]
    copies = []
    for i, (k, mm) in enumerate(offsets):
        slot = (group ^ k) * members + (member ^ mm)
        copies.append(pltpu.make_async_copy(kv_refs[i], kv.at[slot], sems.at[i]))
        copies[-1].start()
    for k in range(groups):
        qs[k] = q_refs[k][...]
    for c in copies:
        c.wait()
    scale = LOG2E / math.sqrt(width)
    tri = lax.broadcasted_iota(jnp.int32, (rows, rows), 0) >= lax.broadcasted_iota(
        jnp.int32, (rows, rows), 1
    )

    def fold(index, state, queries, query_gate, masked):
        best, total, weighted = state
        keys = kv[index, :, :width]
        vals = kv[index, :, width:]
        start = pl.multiple_of(index * rows, rows)
        key_gate = row_ref[:, pl.ds(start, rows)] * LOG2E
        part = lax.dot_general(queries, keys, (((1,), (1,)), ((), ())), preferred_element_type=f32)
        part = part * scale - key_gate
        if masked:
            part = jnp.where(tri, part, -jnp.inf)
        newest = jnp.maximum(best, jnp.max(part, axis=1, keepdims=True) + query_gate)
        factor = jnp.exp2(best - newest)
        weights = jnp.exp2(part - (newest - query_gate))
        total = total * factor + jnp.sum(weights, axis=1, keepdims=True)
        weighted = weighted * factor + jnp.dot(
            weights.astype(bf16), vals, preferred_element_type=f32
        )
        return newest, total, weighted

    for k in range(groups):
        rank = (group ^ k) * members + member
        start = pl.multiple_of(rank * rows, rows)
        queries = qs[k]
        query_gate = col_ref[pl.ds(start, rows), :] * LOG2E
        state = (
            jnp.full((rows, 1), -jnp.inf, f32),
            jnp.zeros((rows, 1), f32),
            jnp.zeros((rows, width), f32),
        )
        state = fold(rank, state, queries, query_gate, True)
        state = lax.fori_loop(
            0,
            rank,
            lambda j, s: fold(j, s, queries, query_gate, False),
            state,
        )
        o_refs[k][...] = (state[2] / state[1]).astype(bf16)


def norm_kernel(parts, ids, x_ref, gain_ref, *outs):
    own = ids[0]
    as_float = x_ref[...].astype(f32)
    center = jnp.mean(as_float, axis=1, keepdims=True)
    shifted = as_float - center
    variance = jnp.mean(jnp.square(shifted), axis=1, keepdims=True)
    normed = (shifted * lax.rsqrt(variance + EPSILON) * gain_ref[...]).astype(bf16)
    width = normed.shape[1] // parts
    scratch = outs[-1]
    scratch[...] = normed
    for k in range(parts):
        at = pl.ds(pl.multiple_of((own ^ k) * width, width), width)
        outs[k][...] = scratch[:, at]


def pick_kernel(parts, experts, capacity, ids, route_ref, *refs):
    own_ep, own_tp = ids[0], ids[1]
    pieces = refs[:parts]
    places_ref = refs[parts]
    outs = refs[parts + 1 : parts + 1 + experts]
    table = refs[-1]
    rows = pieces[0].shape[0]
    for k in range(parts):
        at = pl.ds(pl.multiple_of((own_tp ^ k) * rows, rows), rows)
        table[at, :] = pieces[k][...]
    block = parts * rows
    chosen = route_ref.shape[0]
    names = lax.broadcasted_iota(jnp.int32, (experts, block), 0)
    hits = [(names == route_ref[c : c + 1, :]).astype(f32) for c in range(chosen)]
    before = (
        lax.broadcasted_iota(jnp.int32, (block, block), 0)
        < lax.broadcasted_iota(jnp.int32, (block, block), 1)
    ).astype(bf16)
    running = jnp.dot(sum(hits).astype(bf16), before, preferred_element_type=f32)
    places = []
    for c in range(chosen):
        ranking = jnp.sum(hits[c] * running, axis=0, keepdims=True)
        places.append(route_ref[c : c + 1, :] * capacity + ranking.astype(jnp.int32))
        running = running + hits[c]
    for c in range(chosen):
        places_ref[c : c + 1, :] = places[c]
    for k in range(experts):
        slots = (own_ep ^ k) * capacity + lax.broadcasted_iota(jnp.int32, (capacity, block), 0)
        chosen_rows = sum((slots == places[c]).astype(f32) for c in range(chosen))
        outs[k][...] = jnp.dot(
            chosen_rows.astype(bf16), table[...], preferred_element_type=f32
        ).astype(bf16)


def hidden_kernel(order, ids, *refs):
    parts = len(order)
    pieces = refs[:parts]
    gate_w, up_w = refs[parts : parts + 2]
    out_ref = refs[parts + 2]
    gate_sum, up_sum = refs[parts + 3 :]
    step = pl.program_id(0)

    @pl.when(step == 0)
    def _():
        gate_sum[...] = jnp.zeros_like(gate_sum)
        up_sum[...] = jnp.zeros_like(up_sum)

    for i in range(parts):

        @pl.when(step == i)
        def _():
            gate_sum[...] += jnp.dot(pieces[i][...], gate_w[0], preferred_element_type=f32)
            up_sum[...] += jnp.dot(pieces[i][...], up_w[0], preferred_element_type=f32)

    @pl.when(step == parts - 1)
    def _():
        gate = gate_sum[...]
        out_ref[...] = (gate / (1.0 + jnp.exp(-gate)) * up_sum[...]).astype(bf16)


def gate_up(ids, order, pieces, gate_weight, up_weight):
    parts = len(order)
    rows, depth = pieces[0].shape
    width = gate_weight.shape[2]
    table = jnp.array(order, jnp.int32) ^ ids[1]

    def weight_at(i, sel):
        return (0, sel[i], 0)

    return pl.pallas_call(
        functools.partial(hidden_kernel, order),
        out_shape=jax.ShapeDtypeStruct((rows, width), bf16),
        grid_spec=pltpu.PrefetchScalarGridSpec(
            num_scalar_prefetch=1,
            grid=(parts,),
            in_specs=[pl.BlockSpec((rows, depth), lambda i, sel: (0, 0))] * parts
            + [pl.BlockSpec((1, depth, width), weight_at)] * 2,
            out_specs=pl.BlockSpec((rows, width), lambda i, sel: (0, 0)),
            scratch_shapes=[pltpu.VMEM((rows, width), f32)] * 2,
        ),
        compiler_params=pltpu.CompilerParams(vmem_limit_bytes=56 << 20),
    )(table, *pieces, gate_weight, up_weight)


def product_kernel(order, splits, out_rows, ids, *refs):
    parts = len(order)
    pieces = refs[:parts]
    weight = refs[parts]
    outs = refs[parts + 1 : -1]
    table = refs[-1]

    @pl.when(pl.program_id(0) == 0)
    def _():
        depth = pieces[0].shape[1]
        sub = depth // splits
        for i in range(parts):
            for k in range(splits):
                at = (order[i] ^ ids[0]) * depth + (k ^ ids[1]) * sub
                table[:, pl.ds(pl.multiple_of(at, sub), sub)] = pieces[i][:, k * sub : (k + 1) * sub]

    result = jnp.dot(table[...], weight[...], preferred_element_type=f32).astype(bf16)
    for n, out in enumerate(outs):
        out[...] = result[n * out_rows : (n + 1) * out_rows]


def product(own, sub, order, splits, pieces, weight, out_count):
    rows, depth = pieces[0].shape
    total, width = weight.shape
    tile = math.gcd(width, 256)
    out_rows = rows // out_count
    return pl.pallas_call(
        functools.partial(product_kernel, order, splits, out_rows),
        out_shape=[jax.ShapeDtypeStruct((out_rows, width), bf16)] * out_count,
        grid_spec=pltpu.PrefetchScalarGridSpec(
            num_scalar_prefetch=1,
            grid=(width // tile,),
            in_specs=[pl.BlockSpec((rows, depth), lambda i, sel: (0, 0))] * len(order)
            + [pl.BlockSpec((total, tile), lambda i, sel: (0, i))],
            out_specs=[pl.BlockSpec((out_rows, tile), lambda i, sel: (0, i))] * out_count,
            scratch_shapes=[pltpu.VMEM((rows, total), bf16)],
        ),
        compiler_params=pltpu.CompilerParams(vmem_limit_bytes=56 << 20),
    )(jnp.stack([own, sub]).astype(jnp.int32), *pieces, weight)


def combine_kernel(experts, ids, places_ref, weight_ref, *refs):
    own_ep = ids[0]
    pieces = refs[:experts]
    out_ref = refs[experts]
    capacity = pieces[0].shape[0]
    chosen, block = places_ref.shape
    total = jnp.zeros(out_ref.shape, f32)
    for c in range(chosen):
        picked = jnp.zeros(out_ref.shape, f32)
        for k in range(experts):
            slots = (own_ep ^ k) * capacity + lax.broadcasted_iota(
                jnp.int32, (capacity, block), 0
            )
            hit = (slots == places_ref[c : c + 1, :]).astype(f32).astype(bf16)
            picked += lax.dot_general(
                hit, pieces[k][...], (((0,), (0,)), ((), ())), preferred_element_type=f32
            )
        total += picked * weight_ref[:, c : c + 1]
    out_ref[...] = total.astype(bf16)


def body(
    queries,
    key_rows,
    values,
    forget_log,
    out_weight,
    expert_input,
    norm_gain,
    route_ids,
    route_weights,
    gate_weight,
    up_weight,
    down_weight,
):
    ep, tp = lax.axis_size("ep"), lax.axis_size("tp")
    own_ep, own_tp = lax.axis_index("ep"), lax.axis_index("tp")
    smem = [pl.BlockSpec(memory_space=SMEM)]
    ids = jnp.stack([own_ep, own_tp]).astype(jnp.int32)

    rows_here, model = expert_input.shape
    feature = model // tp
    normed = call(
        functools.partial(norm_kernel, tp),
        [jax.ShapeDtypeStruct((rows_here, feature), bf16)] * tp,
        smem + vm(2),
        (ids[1:], expert_input, norm_gain.reshape(1, -1)),
        out_specs=vm(tp),
        scratch_shapes=[pltpu.VMEM((rows_here, model), bf16)],
    )
    crossed = [normed[0]] + [swap(normed[k], "tp", k) for k in range(1, tp)]
    block, chosen = route_ids.shape
    experts = gate_weight.shape[0] * ep
    capacity = block * chosen * 2 // experts
    picked = call(
        functools.partial(pick_kernel, tp, experts, capacity),
        [jax.ShapeDtypeStruct((chosen, block), jnp.int32)]
        + [jax.ShapeDtypeStruct((capacity, feature), bf16)] * experts,
        smem + vm(1 + tp),
        (ids, route_ids.T, *crossed),
        out_specs=vm(1 + experts),
        scratch_shapes=[pltpu.VMEM((block, feature), bf16)],
    )
    places, leaving = picked[0], picked[1:]

    rows, local = queries.shape
    heads = forget_log.shape[1]
    width = local // heads
    members = ep // heads
    group, member = own_ep // members, own_ep % members
    place = jnp.stack([group, member]).astype(jnp.int32)
    cut = call(
        functools.partial(slice_kernel, width, heads),
        [jax.ShapeDtypeStruct((rows, width), bf16)] * heads
        + [jax.ShapeDtypeStruct((rows, 2 * width), bf16)] * heads,
        smem + vm(3),
        (place, queries, key_rows, values),
        out_specs=vm(2 * heads),
    )
    head_q = [cut[0]] + [swap(cut[k], "ep", k * members) for k in range(1, heads)]

    arrived = [leaving[0]] + [swap(leaving[k], "ep", k) for k in range(1, ep)]
    near, far = arrived[: ep // 2], arrived[ep // 2 :]
    pairs = list(cut[heads:])
    pairs, far = lax.optimization_barrier((pairs, far))
    offsets, kv = [], []
    for k in range(heads):
        piece = pairs[0] if k == 0 else swap(pairs[k], "ep", k * members)
        order, items = doubled(piece, "ep", members)
        offsets += [(k, mm) for mm in order]
        kv += items
    gate_row = lax.dynamic_slice_in_dim(forget_log.T, group, 1, 0)
    gate_col = gate_row.reshape(-1, 1)
    out = call(
        functools.partial(flash_kernel, heads, members, offsets, rows, width),
        [jax.ShapeDtypeStruct((rows, width), bf16)] * heads,
        smem
        + vm(heads)
        + [pl.BlockSpec(memory_space=HBM)] * len(kv)
        + vm(2),
        (place, *head_q, *kv, gate_row, gate_col),
        out_specs=vm(heads),
        scratch_shapes=[
            pltpu.VMEM((ep, rows, 2 * width), bf16),
            pltpu.VMEM((heads, rows, width), bf16),
            pltpu.SemaphoreType.DMA((len(kv),)),
        ],
    )
    back = [out[0]] + [swap(out[k], "ep", k * members) for k in range(1, heads)]
    order, attended = doubled(jnp.concatenate(back, axis=1), "tp", tp)
    (mixer_out,) = product(own_tp, group, order, heads, attended, out_weight, 1)

    returned = []
    for half in (near, far):
        order, tokens = doubled(jnp.concatenate(half, axis=0), "tp", tp)
        hidden = gate_up(ids, order, tokens, gate_weight, up_weight)
        order, slices = doubled(hidden, "tp", tp)
        returned += product(
            own_tp, jnp.zeros_like(own_tp), order, 1, slices, down_weight[0], len(half)
        )
    landed = [returned[0]] + [swap(returned[k], "ep", k) for k in range(1, ep)]
    expert_out = call(
        functools.partial(combine_kernel, experts),
        jax.ShapeDtypeStruct((block, out_weight.shape[1]), bf16),
        smem + vm(2 + experts),
        (ids, places, route_weights, *landed),
        out_specs=pl.BlockSpec(memory_space=VMEM),
    )
    return mixer_out, expert_out


def solution(mesh):
    placed = (
        P("ep", "tp"),
        P("ep", "tp"),
        P("ep", "tp"),
        P(None, "tp"),
        P(None, "tp"),
        P(("ep", "tp"), None),
        P(),
        P("ep", None),
        P("ep", None),
        P("ep", None, "tp"),
        P("ep", None, "tp"),
        P("ep", None, "tp"),
    )
    return jax.shard_map(
        body, mesh=mesh, in_specs=placed, out_specs=(P("ep", "tp"), P("ep", "tp")), check_vma=False
    )
```
